32 devices in a mesh: tp: 8 (over z, core), dp: 4 (over y, x).
Axes of the slice: x: 2, y: 2, z: 4, core: 2. Of those that a mesh axis runs over, the one named last changes fastest.
Arguments:
- tokens: bfloat16 [128, 2048], P(None, 'dp'), may hold values from -21 to 21
- lengths: int32 [8], P('dp'), may hold values from 1 to 16, 42 in all
- input_norm_scale: float32 [2, 2048], P(None, 'dp'), may hold values from 0.1 to 1.9
- gate_input_weight: bfloat16 [2, 2048, 2, 2048], P(None, 'dp', None, 'tp'), may hold values from -0.125 to 0.125
- maps_weight: bfloat16 [2, 2048, 2, 512], P(None, 'dp', None, 'tp'), may hold values from -0.125 to 0.125
- step_weight: bfloat16 [2, 2048, 32], P(None, 'dp', 'tp'), may hold values from -0.125 to 0.125
- input_tap_weight: bfloat16 [2, 4, 2048], P(None, None, 'tp'), may hold values from -3 to 3
- map_tap_weight: bfloat16 [2, 4, 2, 512], P(None, None, None, 'tp'), may hold values from -3 to 3
- step_size_bias: float32 [2, 32], P(None, 'tp'), may hold values from -4 to -1
- decay_rate_logarithm: float32 [2, 32], P(None, 'tp'), may hold values from -2 to 2.5
- direct_path_weight: float32 [2, 32], P(None, 'tp'), may hold values from 0.25 to 2.5
- head_norm_scale: float32 [2, 2048], P(None, 'tp'), may hold values from 0.1 to 1.9
- output_weight: bfloat16 [2, 2048, 2048], P(None, 'tp', 'dp'), may hold values from -0.125 to 0.125
- convolution_input_cache: bfloat16 [2, 8, 3, 2048], P(None, 'dp', None, 'tp'), may hold values from -6 to 6
- convolution_map_cache: bfloat16 [2, 8, 3, 2, 512], P(None, 'dp', None, None, 'tp'), may hold values from -6 to 6
- recurrent_state: float32 [2, 8, 32, 64, 128], P(None, 'dp', 'tp'), may hold values from -6 to 6
- extra_log_decay: float32 [2, 8, 16, 32], P(None, 'dp', None, 'tp'), may hold values from -0.7 to 0, as said below
Outputs:
- stream_out: float32 [128, 2048], P(None, 'dp')
- conv_input_out: bfloat16 [2, 8, 3, 2048], P(None, 'dp', None, 'tp')
- conv_maps_out: bfloat16 [2, 8, 3, 2, 512], P(None, 'dp', None, None, 'tp')
- ssm_out: float32 [2, 8, 32, 64, 128], P(None, 'dp', 'tp')
The draws below stay inside these ranges and needn't reach their ends.
Inputs may be any that keep to these rules, and one draw needn't show every extreme that they name: `extra_log_decay`: zero at most slots, a drop of a fifth to a half of the state at a few.
All inputs are finite; a program needn't handle non-finite values. No bound on the sum of `lengths` on one device may be relied on, other than what follows from the above.
Results may differ from the reference program's by a relative error of at most 0.04.
Values may be sent and summed in bfloat16 or wider, within the bound.
A program may use at most 64 MiB of HBM per device.

```python
import math
import jax
import jax.numpy as jnp
import numpy as np
from jax import lax

D = 2048
STATE_HEADS = 32
P_SIZE = 64
N = 128
G = 4
CONV = 4
TOKEN_SLOTS = 16
MIXER_LAYERS = 2
INNER = 2048
GN = 512
SEQUENCE_COUNT = 8
TOKENS = 128
DP_ROWS = 512
N_DP = 4


def draw_tokens(key, part):
    random_key_first, random_key_second = jax.random.split(key, 2)
    base_draw = jnp.clip(jax.random.normal(random_key_first, (TOKENS, D), jnp.float32), -4.0, 4.0)
    column = jnp.exp(jnp.linspace(math.log(0.5), math.log(3.0), D)) * jax.random.uniform(random_key_second, (D,), jnp.float32, 0.7, 1.0)
    return (base_draw * column[None, :]).astype(jnp.bfloat16)


def draw_extra_log_decay(key, part):
    random_key_first, random_key_second = jax.random.split(key)
    spike_hits = jax.random.randint(random_key_first, (MIXER_LAYERS, SEQUENCE_COUNT, TOKEN_SLOTS, STATE_HEADS), 0, 12) == 0
    spike_depth = jax.random.uniform(random_key_second, (MIXER_LAYERS, SEQUENCE_COUNT, TOKEN_SLOTS, STATE_HEADS), jnp.float32, math.log(0.5), math.log(0.8))
    return jnp.where(spike_hits, spike_depth, 0.0).astype(jnp.float32)


def level_of(own_key, dims, cuts, smallest, largest):
    level, own = 1.0, jax.random.fold_in(own_key, 6)
    for axis_at, shards_of in cuts:
        steps = jnp.exp(jax.random.uniform(jax.random.fold_in(own, axis_at), (shards_of,), jnp.float32, smallest / len(cuts), largest / len(cuts)))
        level = level * jnp.repeat(steps, dims[axis_at] // shards_of).reshape([-1 if axis == axis_at else 1 for axis in range(len(dims))])
    return level


def split_up(number_of, total, reach, slope):
    loads = [(1 << 20) // math.isqrt(grade ** slope) + 1 for grade in range(2, number_of + 1)]
    surplus, holding = total - reach - (number_of - 1), [1] * (number_of - 1)
    while surplus > 0:
        candidates = [i for i in range(number_of - 1) if holding[i] < reach]
        mass, remaining = sum([loads[i] for i in candidates]), surplus
        for i in candidates:
            more = min(reach - holding[i], max(1, remaining * loads[i] // mass), surplus)
            holding[i] = holding[i] + more
            surplus = surplus - more
    return np.array([reach] + holding)


def ragged(stream_key, number_of, total, most, skew):
    if number_of == 2:
        one = jax.random.randint(stream_key, (), max(1, total - most), min(most, total - 1) + 1)
        return jnp.stack([one, total - one])
    sizes = jnp.asarray(split_up(number_of, total, most, skew), jnp.int32)
    twos = (number_of - 1) // 2
    source_of, taker = sizes[1:1 + 2 * twos:2], sizes[2:2 + 2 * twos:2]
    room = jnp.minimum(source_of - 1, most - taker)
    shifted = jax.random.randint(jax.random.fold_in(stream_key, 1), (twos,), 0, 1 << 20) % (room + 1)
    sizes = sizes.at[1:1 + 2 * twos:2].set(source_of - shifted).at[2:2 + 2 * twos:2].set(taker + shifted)
    return sizes[jax.random.permutation(jax.random.fold_in(stream_key, 2), number_of)]


def scatter_about(own_key, dims, spread, bound, pieces=(), held_as=jnp.bfloat16):
    gain = level_of(own_key, dims, pieces, -0.22, 0.18) if pieces else 1.0
    entries = jax.random.normal(own_key, dims, jnp.float32) * spread * gain
    return jnp.minimum(jnp.maximum(entries, -bound), bound).astype(held_as)


def setup_inputs(seed: int = 0) -> dict:
    arg_keys = jax.random.split(jax.random.key(seed), 18)
    return {
        "tokens": draw_tokens(jax.random.fold_in(arg_keys[17], 71), 0),
        "lengths": ragged(arg_keys[1], SEQUENCE_COUNT, SEQUENCE_COUNT * TOKEN_SLOTS // 3, TOKEN_SLOTS, 2).astype(jnp.int32),
        "input_norm_scale": jnp.clip(1.0 + 0.18 * jax.random.normal(arg_keys[2], (MIXER_LAYERS, D), jnp.float32), 0.1, 1.9),
        "gate_input_weight": scatter_about(arg_keys[3], (MIXER_LAYERS, D, 2, INNER), D ** -0.5, 0.125, ((1, 4), (3, 8))),
        "maps_weight": scatter_about(arg_keys[4], (MIXER_LAYERS, D, 2, GN), D ** -0.5, 0.125, ((1, 4), (3, 8))),
        "step_weight": scatter_about(arg_keys[5], (MIXER_LAYERS, D, STATE_HEADS), D ** -0.5, 0.125, ((1, 4), (2, 8))),
        "input_tap_weight": scatter_about(arg_keys[6], (MIXER_LAYERS, CONV, INNER), CONV ** -0.5, 3.0, ((2, 8),)),
        "map_tap_weight": scatter_about(arg_keys[7], (MIXER_LAYERS, CONV, 2, GN), CONV ** -0.5, 3.0, ((3, 8),)),
        "step_size_bias": jnp.clip(-4.0 + 3.0 * jax.random.uniform(arg_keys[8], (MIXER_LAYERS, STATE_HEADS), jnp.float32) ** level_of(arg_keys[8], (MIXER_LAYERS, STATE_HEADS), ((1, 8),), -0.2, 0.2), -4.0, -1.0),
        "decay_rate_logarithm": jnp.clip(-2.0 + 4.5 * jax.random.uniform(arg_keys[9], (MIXER_LAYERS, STATE_HEADS), jnp.float32) ** level_of(arg_keys[9], (MIXER_LAYERS, STATE_HEADS), ((1, 8),), -0.2, 0.2), -2.0, 2.5),
        "direct_path_weight": jnp.clip(jnp.exp(math.log(2.5) - 2.3025851 * jax.random.uniform(arg_keys[10], (MIXER_LAYERS, STATE_HEADS), jnp.float32) ** level_of(arg_keys[10], (MIXER_LAYERS, STATE_HEADS), ((1, 8),), -0.2, 0.2)), 0.25, 2.5),
        "head_norm_scale": jnp.clip(1.0 + 0.18 * jax.random.normal(arg_keys[11], (MIXER_LAYERS, INNER), jnp.float32), 0.1, 1.9),
        "output_weight": scatter_about(arg_keys[12], (MIXER_LAYERS, INNER, D), INNER ** -0.5, 0.125, ((1, 8), (2, 4))),
        "convolution_input_cache": scatter_about(arg_keys[13], (MIXER_LAYERS, SEQUENCE_COUNT, 3, INNER), 1.0, 6.0, ((1, 4), (3, 8))),
        "convolution_map_cache": scatter_about(arg_keys[14], (MIXER_LAYERS, SEQUENCE_COUNT, 3, 2, GN), 1.0, 6.0, ((1, 4), (4, 8))),
        "recurrent_state": scatter_about(arg_keys[15], (MIXER_LAYERS, SEQUENCE_COUNT, STATE_HEADS, P_SIZE, N), 1.0, 6.0, ((1, 4), (2, 8)), jnp.float32),
        "extra_log_decay": draw_extra_log_decay(jax.random.fold_in(arg_keys[17], 71), 0),
    }


epsilon = 1e-06
highest = lax.Precision.HIGHEST

def conv_step(previous, incoming, weights, lengths):
    padded = jnp.concatenate([previous, incoming], axis=1).astype(jnp.float32)
    taps = weights.shape[0]
    fresh_tokens = incoming.shape[1]
    filtered = padded[:, :fresh_tokens] * weights[0].astype(jnp.float32)
    for tap_index in range(1, taps):
        filtered = filtered + padded[:, tap_index:tap_index + fresh_tokens] * weights[tap_index].astype(jnp.float32)
    position = jnp.arange(fresh_tokens + taps - 1, dtype=jnp.int32)
    wanted = lengths[:, None] + jnp.arange(taps - 1, dtype=jnp.int32)[None, :]
    chooser = (position[None, None, :] == wanted[:, :, None]).astype(jnp.float32)
    kept_rows = jnp.einsum('skp,sp...->sk...', chooser, padded, precision=highest)
    return (jax.nn.silu(filtered), kept_rows.astype(jnp.bfloat16))

def ssd_block(head_input, head_gate, head_step_size, decay_logarithm, write_map, read_map, state_old, skip, gain_heads):
    decay_sum = jnp.cumsum(decay_logarithm, axis=1)
    slots = decay_logarithm.shape[1]
    causal = jnp.arange(slots)[:, None] >= jnp.arange(slots)[None, :]
    decay_gap = decay_sum[:, :, None, :] - decay_sum[:, None, :, :]
    segment = jnp.exp(jnp.where(causal[None, :, :, None], decay_gap, -jnp.inf))
    intersection = jnp.einsum('slhn,smhn->slmh', read_map, write_map, precision=highest)
    within = jnp.einsum('slmh,smh,smhp->slhp', intersection * segment, head_step_size, head_input, precision=highest)
    carried = jnp.einsum('slhn,shpn->slhp', read_map, state_old, precision=highest) * jnp.exp(decay_sum)[..., None]
    to_end = jnp.exp(decay_sum[:, -1:, :] - decay_sum)
    state_new = jnp.exp(decay_sum[:, -1])[..., None, None] * state_old + jnp.einsum('smhn,smh,smhp->shpn', write_map, to_end * head_step_size, head_input, precision=highest)
    mixed_out = within + carried + skip[:, None] * head_input
    mixed_out = mixed_out * jax.nn.silu(head_gate)
    mixed_out = mixed_out * lax.rsqrt(lax.optimization_barrier(jnp.mean(mixed_out * mixed_out, axis=-1, keepdims=True)) + epsilon) * gain_heads
    return (mixed_out, state_new)

def reference(tokens, lengths, input_norm_scale, gate_input_weight, maps_weight, step_weight, input_tap_weight, map_tap_weight, step_size_bias, decay_rate_logarithm, direct_path_weight, head_norm_scale, output_weight, convolution_input_cache, convolution_map_cache, recurrent_state, extra_log_decay):
    stream = tokens.astype(jnp.float32)
    active_mask = (jnp.arange(TOKEN_SLOTS, dtype=jnp.int32)[None, :] < lengths[:, None]).astype(jnp.float32)
    input_states, map_states, ssm_states = ([], [], [])
    per_group = STATE_HEADS // G
    for layer_number in range(MIXER_LAYERS):
        stream_f = stream
        factor = lax.rsqrt(lax.optimization_barrier(jnp.sum(stream_f * stream_f, axis=1, keepdims=True)) / D + epsilon)
        normed = (stream_f * input_norm_scale[layer_number]).astype(jnp.bfloat16)
        weight_all = jnp.concatenate([gate_input_weight[layer_number].reshape(D, 2 * INNER), maps_weight[layer_number].reshape(D, 2 * GN), step_weight[layer_number]], axis=1)
        total_cols = weight_all.shape[1]
        row_pieces = normed.reshape(TOKENS, N_DP, DP_ROWS).transpose(1, 0, 2)
        weight_pieces = weight_all.reshape(N_DP, DP_ROWS, total_cols)

        def add_block(running, pair_item):
            partial_prod = jnp.dot(pair_item[0], pair_item[1], preferred_element_type=jnp.float32)
            rounded = lax.optimization_barrier(partial_prod.astype(jnp.bfloat16))
            return (running + rounded.astype(jnp.float32), None)
        proj_sum, _ = lax.scan(add_block, jnp.zeros((TOKENS, total_cols), jnp.float32), (row_pieces, weight_pieces))
        projected = (proj_sum * factor).astype(jnp.bfloat16)
        gate_input = projected[:, :2 * INNER].reshape(SEQUENCE_COUNT, TOKEN_SLOTS, 2, INNER)
        map_input = projected[:, 2 * INNER:2 * INNER + 2 * GN].reshape(SEQUENCE_COUNT, TOKEN_SLOTS, 2, GN)
        step_raw = projected[:, 2 * INNER + 2 * GN:].reshape(SEQUENCE_COUNT, TOKEN_SLOTS, STATE_HEADS)
        conv_input, input_kept = conv_step(convolution_input_cache[layer_number], gate_input[:, :, 1], input_tap_weight[layer_number], lengths)
        maps_f, maps_kept = conv_step(convolution_map_cache[layer_number], map_input, map_tap_weight[layer_number], lengths)
        maps = maps_f.astype(jnp.bfloat16)
        write_groups = maps[:, :, 0].reshape(SEQUENCE_COUNT, TOKEN_SLOTS, N, G).transpose(0, 1, 3, 2)
        read_groups = maps[:, :, 1].reshape(SEQUENCE_COUNT, TOKEN_SLOTS, N, G).transpose(0, 1, 3, 2)
        write_map = jnp.repeat(write_groups, per_group, axis=2).astype(jnp.float32)
        read_map = jnp.repeat(read_groups, per_group, axis=2).astype(jnp.float32)
        head_step_size = jax.nn.softplus(step_raw.astype(jnp.float32) + step_size_bias[layer_number]) * active_mask[..., None]
        decay_logarithm = head_step_size * -jnp.exp(decay_rate_logarithm[layer_number]) + extra_log_decay[layer_number] * active_mask[..., None]
        head_input = conv_input.reshape(SEQUENCE_COUNT, TOKEN_SLOTS, STATE_HEADS, P_SIZE)
        head_gate = gate_input[:, :, 0].astype(jnp.float32).reshape(SEQUENCE_COUNT, TOKEN_SLOTS, STATE_HEADS, P_SIZE)
        mixed_out, state_new = ssd_block(head_input, head_gate, head_step_size, decay_logarithm, write_map, read_map, recurrent_state[layer_number], direct_path_weight[layer_number], head_norm_scale[layer_number].reshape(STATE_HEADS, P_SIZE))
        head_out = (mixed_out * active_mask[:, :, None, None]).astype(jnp.bfloat16).reshape(TOKENS, INNER)
        projected_out = jnp.dot(head_out, output_weight[layer_number], preferred_element_type=jnp.float32)
        stream = stream_f + projected_out
        input_states.append(input_kept)
        map_states.append(maps_kept)
        ssm_states.append(state_new)
    return (stream, jnp.stack(input_states), jnp.stack(map_states), jnp.stack(ssm_states))
```

```python
import functools

import jax
import jax.numpy as jnp
import numpy as np
from jax import lax
from jax.experimental import pallas as pl
from jax.experimental.pallas import tpu as pltpu
from jax.sharding import PartitionSpec as P

EPS = 1e-06
LANES = 128
FRONT = 8
HIGHEST = lax.Precision.HIGHEST
F32, BF16 = jnp.float32, jnp.bfloat16


def up(n):
    return -(-n // LANES) * LANES


def dot(a, b, ca=1, cb=0, precision=None):
    return lax.dot_general(
        a, b, (((ca,), (cb,)), ((), ())), precision=precision, preferred_element_type=F32
    )


def kernel(
    n_tp, n_dp, d_model, heads, groups, slots, seqs, hp_cols, map_cols,
    lens, x, scale, w, taps, cache, par, hv, extra, state, wout, sel, sel2, tri, ex, ext, ones,
    stream, kept, ssm,
    a_send, a_recv, m_send, m_recv, h_send, h_recv, o_send, o_recv, n_send, n_recv, padded,
    a_ss, a_rs, m_ss, m_rs, h_ss, h_rs, o_ss, o_rs, n_ss, n_rs,
):
    tp, dp = lax.axis_index("tp"), lax.axis_index("dp")
    layers = w.shape[0]
    rows = seqs * slots
    taps_n = taps.shape[1]
    keep = taps_n - 1
    zc = up(hp_cols)
    ng = map_cols // groups
    n_state = state.shape[-1]
    cut = stream.shape[0] // n_tp
    per = rows // cut
    head_size = hp_cols // heads

    barrier = pltpu.get_barrier_semaphore()
    for k in range(1, n_dp):
        pl.semaphore_signal(barrier, inc=1, device_id={"dp": lax.rem(dp + k, n_dp)})
    for k in range(1, n_tp):
        pl.semaphore_signal(barrier, inc=1, device_id={"tp": lax.rem(tp + k, n_tp)})

    stream[...] = x[...].astype(F32)
    slot = lax.broadcasted_iota(jnp.int32, (slots, 1), 0)
    mask = jnp.concatenate([(slot < lens[s]).astype(F32) for s in range(seqs)], axis=0)
    lane = lax.broadcasted_iota(jnp.int32, (1, LANES), 1)
    r_id = lax.broadcasted_iota(jnp.int32, (rows, rows), 0)
    c_id = lax.broadcasted_iota(jnp.int32, (rows, rows), 1)
    causal = tri[...] > 0.5
    padded[...] = jnp.zeros_like(padded)
    sends = []

    def copy(src, dst, ss, rs, where):
        return pltpu.make_async_remote_copy(
            src_ref=src, dst_ref=dst, send_sem=ss, recv_sem=rs, device_id=where
        )

    for l in range(layers):
        st = stream[...]
        squares = jnp.sum(st * st, axis=1, keepdims=True)
        normed = (st * scale[l : l + 1, :]).astype(BF16)
        part = dot(normed, w[l])
        tail = part[:, part.shape[1] - LANES :]
        high = squares.astype(BF16).astype(F32)
        tail = jnp.where(lane == LANES - 2, high, jnp.where(lane == LANES - 1, squares - high, tail))
        part = jnp.concatenate([part[:, : part.shape[1] - LANES], tail], axis=1).astype(BF16)
        for b in range(n_dp):
            a_send[l, b] = part[b * rows : (b + 1) * rows]
        if l == 0:
            pl.semaphore_wait(barrier, n_dp - 1 + n_tp - 1)
        flights = []
        for k in range(1, n_dp):
            to = lax.rem(dp + k, n_dp)
            c = copy(a_send.at[l, to], a_recv.at[l, k - 1], a_ss.at[l, k - 1], a_rs.at[l, k - 1], {"dp": to})
            c.start()
            flights.append(c)
        sends += flights
        acc = a_send[l, dp].astype(F32)
        for k, c in enumerate(flights):
            c.wait_recv()
            acc = acc + a_recv[l, k].astype(F32)
        tail = acc[:, acc.shape[1] - LANES :]
        squares = tail[:, LANES - 2 : LANES - 1] + tail[:, LANES - 1 : LANES]
        factor = lax.rsqrt(squares / d_model + EPS)
        proj = (acc * factor).astype(BF16).astype(F32)

        conv_w = taps.shape[2]
        pieces = []
        for s in range(seqs):
            padded[s, FRONT - keep : FRONT, :] = cache[l, s].astype(F32)
            padded[s, FRONT : FRONT + slots, :] = proj[s * slots : (s + 1) * slots, zc : zc + conv_w]
            total = padded[s, FRONT - keep : FRONT - keep + slots, :] * taps[l, 0:1, :]
            for t in range(1, taps_n):
                at = FRONT - keep + t
                total = total + padded[s, at : at + slots, :] * taps[l, t : t + 1, :]
            pieces.append(total)
        filtered = jnp.concatenate(pieces, axis=0)
        filtered = filtered * jax.nn.sigmoid(filtered)
        maps = filtered[:, conv_w - up(2 * map_cols) :].astype(BF16)
        sorted_maps = dot(sel[...], maps, 1, 1)
        for g in range(groups):
            m_send[l, g] = sorted_maps[g * 2 * ng : (g + 1) * 2 * ng, :].astype(BF16)

        def group_of(rank):
            return rank * heads // (heads * n_tp // groups)

        flights = []
        for k in range(1, n_tp):
            to = lax.rem(tp + k, n_tp)
            c = copy(m_send.at[l, group_of(to)], m_recv.at[l, tp], m_ss.at[l, k - 1], m_rs.at[l, k - 1], {"tp": to})
            c.start()
            flights.append(c)
        sends += flights
        m_recv[l, tp] = m_send[l, group_of(tp)]

        for s in range(seqs):
            pick = lax.broadcasted_iota(jnp.int32, (8, FRONT + slots), 0)
            place = lax.broadcasted_iota(jnp.int32, (8, FRONT + slots), 1)
            chooser = ((place == pick + lens[s] + (FRONT - keep)) & (pick < keep)).astype(BF16)
            kept[l, s] = dot(chooser, padded[s].astype(BF16)).astype(BF16)
        raw = proj[:, proj.shape[1] - LANES :] + par[l, 0:1, :]
        step = (jnp.maximum(raw, 0.0) + jnp.log1p(jnp.exp(-jnp.abs(raw)))) * mask
        step = jnp.where(lane < heads, step, 0.0)
        logdec = extra[l] * mask - step * jnp.exp(par[l, 1:2, :])
        logdec = jnp.where(lane < heads, logdec, 0.0)
        sums = dot(tri[...], logdec, precision=HIGHEST)
        sums_t = sums.T
        step_t = step.T
        both = dot(jnp.concatenate([sums, step], axis=0), ex[...], precision=HIGHEST)
        sums_x, step_x = both[:rows], both[rows:]
        inp = filtered[:, :hp_cols]
        gate = proj[:, :hp_cols]
        last_x = jnp.concatenate(
            [
                jnp.broadcast_to(sums_x[(s + 1) * slots - 1 : (s + 1) * slots, :], (slots, hp_cols))
                for s in range(seqs)
            ],
            axis=0,
        )
        weighted = (jnp.exp(last_x - sums_x) * step_x * inp).astype(BF16)
        inp_b = inp.astype(BF16)
        grow = jnp.exp(sums_x)
        direct = hv[l, 0:1, :] * inp
        gate = gate * jax.nn.sigmoid(gate)
        rows_sum = dot(ext[...], sums, 1, 1, precision=HIGHEST)
        segs = []
        for h in range(heads):
            gap = sums[:, h : h + 1] - sums_t[h : h + 1, :]
            segs.append(jnp.exp(jnp.where(causal, gap, -jnp.inf)) * step_t[h : h + 1, :])

        for c in flights:
            c.wait_recv()
        got = m_recv[l].astype(F32).reshape(n_tp * 2 * ng, rows)
        both_maps = dot(got.T.astype(BF16), sel2[...]).astype(BF16)
        b_map, c_map = both_maps[:, :n_state], both_maps[:, n_state:]
        cross = dot(c_map, b_map, 1, 1)
        within = jnp.concatenate(
            [
                dot((cross * segs[h]).astype(BF16), inp_b[:, h * head_size : (h + 1) * head_size])
                for h in range(heads)
            ],
            axis=1,
        )
        carried = jnp.concatenate(
            [
                dot(c_map[s * slots : (s + 1) * slots], state[l, s].astype(BF16), 1, 1)
                for s in range(seqs)
            ],
            axis=0,
        )
        read = (within + carried * grow + direct) * gate
        power = read * read
        p_hi = power.astype(BF16)
        p_lo = (power - p_hi.astype(F32)).astype(BF16)
        mean = (dot(p_hi, ones[...]) + dot(p_lo, ones[...])) / head_size
        headout = (read * lax.rsqrt(mean + EPS) * hv[l, 1:2, :] * mask).astype(BF16)
        h_send[l] = headout
        flights = []
        for k in range(1, n_dp):
            to = lax.rem(dp + k, n_dp)
            c = copy(h_send.at[l], h_recv.at[l, k - 1], h_ss.at[l, k - 1], h_rs.at[l, k - 1], {"dp": to})
            c.start()
            flights.append(c)
        sends += flights

        def push(value, block):
            out = dot(value, wout[l]).astype(BF16)
            for i in range(per):
                to = block * per + i
                o_send[l, to] = out[i * cut : (i + 1) * cut]

                @pl.when(to != tp)
                def _():
                    copy(o_send.at[l, to], o_recv.at[l, tp], o_ss.at[l, to], o_rs.at[l, tp], {"tp": to}).start()

        push(headout, dp)
        for s in range(seqs):
            at = slice(s * slots, (s + 1) * slots)
            fresh = dot(weighted[at], b_map[at], 0, 0)
            end = (s + 1) * slots - 1
            ssm[l, s] = jnp.exp(rows_sum[:, end : end + 1]) * state[l, s] + fresh
        for k, c in enumerate(flights):
            c.wait_recv()
            push(h_recv[l, k], lax.rem(dp + n_dp - k - 1, n_dp))
        total = o_send[l, tp].astype(F32)
        for k in range(1, n_tp):
            src = lax.rem(tp + n_tp - k, n_tp)
            copy(o_send.at[l, src], o_recv.at[l, src], o_ss.at[l, src], o_rs.at[l, src], {"tp": src}).wait_recv()
            total = total + o_recv[l, src].astype(F32)
        fresh = total.astype(BF16)
        n_send[l] = fresh
        n_recv[l, tp] = fresh
        flights = []
        for k in range(1, n_tp):
            to = lax.rem(tp + k, n_tp)
            c = copy(n_send.at[l], n_recv.at[l, tp], n_ss.at[l, k - 1], n_rs.at[l, k - 1], {"tp": to})
            c.start()
            flights.append(c)
        sends += flights
        for c in flights:
            c.wait_recv()
        stream[...] += n_recv[l].astype(F32).reshape(stream.shape)

    for c in sends:
        c.wait_send()
    for l in range(layers):
        for k in range(1, n_tp):
            to = lax.rem(tp + k, n_tp)
            copy(o_send.at[l, to], o_recv.at[l, tp], o_ss.at[l, to], o_rs.at[l, tp], {"tp": to}).wait_send()


def body(
    n_tp, n_dp,
    tokens, lengths, input_norm_scale, gate_input_weight, maps_weight, step_weight,
    input_tap_weight, map_tap_weight, step_size_bias, decay_rate_logarithm, direct_path_weight,
    head_norm_scale, output_weight, convolution_input_cache, convolution_map_cache,
    recurrent_state, extra_log_decay,
):
    layers, seqs, slots, heads = extra_log_decay.shape
    head_size, n_state = recurrent_state.shape[3:]
    hp_cols = heads * head_size
    map_cols = maps_weight.shape[3]
    groups = map_cols * n_tp // n_state
    ng = map_cols // groups
    rows = seqs * slots
    d_here = tokens.shape[1]
    keep = convolution_input_cache.shape[2]

    def wide(a):
        pad = up(a.shape[-1]) - a.shape[-1]
        return a if pad == 0 else jnp.pad(a, [(0, 0)] * (a.ndim - 1) + [(0, pad)])

    w = jnp.concatenate(
        [
            wide(gate_input_weight[:, :, 0]),
            wide(gate_input_weight[:, :, 1]),
            wide(maps_weight.reshape(layers, d_here, 2 * map_cols)),
            wide(step_weight),
        ],
        axis=2,
    )
    taps = jnp.concatenate(
        [wide(input_tap_weight), wide(map_tap_weight.reshape(layers, -1, 2 * map_cols))], axis=2
    ).astype(F32)
    cache = jnp.concatenate(
        [
            wide(convolution_input_cache),
            wide(convolution_map_cache.reshape(layers, seqs, keep, 2 * map_cols)),
        ],
        axis=3,
    )
    par = wide(jnp.stack([step_size_bias, decay_rate_logarithm], axis=1))
    hv = jnp.stack([jnp.repeat(direct_path_weight, head_size, axis=1), head_norm_scale], axis=1)
    extra = wide(extra_log_decay.reshape(layers, rows, heads))
    state = recurrent_state.reshape(layers, seqs, hp_cols, n_state)

    sel = np.zeros((2 * map_cols, up(2 * map_cols)), np.float32)
    for g in range(groups):
        for which in range(2):
            for j in range(ng):
                sel[g * 2 * ng + which * ng + j, which * map_cols + groups * j + g] = 1
    sel2 = np.zeros((n_tp * 2 * ng, 2 * n_state), np.float32)
    for src in range(n_tp):
        for which in range(2):
            for j in range(ng):
                sel2[src * 2 * ng + which * ng + j, which * n_state + src * ng + j] = 1
    tri = np.kron(np.eye(seqs), np.tril(np.ones((slots, slots)))).astype(np.float32)
    ex = np.zeros((LANES, hp_cols), np.float32)
    ex[:heads] = np.kron(np.eye(heads), np.ones((1, head_size)))
    ones = np.kron(np.eye(heads), np.ones((head_size, head_size))).astype(np.float32)

    vmem = pl.BlockSpec(memory_space=pltpu.VMEM)
    wide_cols = w.shape[2]
    conv_w = taps.shape[2]
    cut = tokens.shape[0] // n_tp
    sems = lambda n: pltpu.SemaphoreType.DMA((layers, n))
    args = [
        tokens, input_norm_scale, w, taps, cache, par, hv, extra, state, output_weight,
        jnp.asarray(sel, BF16), jnp.asarray(sel2, BF16), jnp.asarray(tri), jnp.asarray(ex),
        jnp.asarray(ex.T.copy()), jnp.asarray(ones, BF16),
    ]
    stream, kept, ssm = pl.pallas_call(
        functools.partial(
            kernel, n_tp, n_dp, d_here * n_dp, heads, groups, slots, seqs, hp_cols, map_cols
        ),
        out_shape=(
            jax.ShapeDtypeStruct(tokens.shape, F32),
            jax.ShapeDtypeStruct((layers, seqs, 8, conv_w), BF16),
            jax.ShapeDtypeStruct(state.shape, F32),
        ),
        in_specs=[pl.BlockSpec(memory_space=pltpu.SMEM)] + [vmem] * len(args),
        out_specs=(vmem, vmem, vmem),
        scratch_shapes=[
            pltpu.VMEM((layers, n_dp, rows, wide_cols), BF16),
            pltpu.VMEM((layers, n_dp - 1, rows, wide_cols), BF16),
            pltpu.VMEM((layers, groups, 2 * ng, rows), BF16),
            pltpu.VMEM((layers, n_tp, 2 * ng, rows), BF16),
            pltpu.VMEM((layers, rows, hp_cols), BF16),
            pltpu.VMEM((layers, n_dp - 1, rows, hp_cols), BF16),
            pltpu.VMEM((layers, n_tp, cut, d_here), BF16),
            pltpu.VMEM((layers, n_tp, cut, d_here), BF16),
            pltpu.VMEM((layers, cut, d_here), BF16),
            pltpu.VMEM((layers, n_tp, cut, d_here), BF16),
            pltpu.VMEM((seqs, FRONT + slots, conv_w), F32),
            sems(n_dp - 1), sems(n_dp - 1), sems(n_tp - 1), sems(n_tp - 1), sems(n_dp - 1),
            sems(n_dp - 1), sems(n_tp), sems(n_tp), sems(n_tp - 1), sems(n_tp - 1),
        ],
        compiler_params=pltpu.CompilerParams(
            collective_id=0, has_side_effects=True, vmem_limit_bytes=48 * 2**20
        ),
        name="mixer",
    )(lengths, *args)
    conv_in = kept[:, :, :keep, :hp_cols]
    start = conv_w - up(2 * map_cols)
    conv_maps = kept[:, :, :keep, start : start + 2 * map_cols].reshape(
        layers, seqs, keep, 2, map_cols
    )
    return stream, conv_in, conv_maps, ssm.reshape(recurrent_state.shape)


def solution(mesh):
    placed = (
        P(None, "dp"),
        P("dp"),
        P(None, "dp"),
        P(None, "dp", None, "tp"),
        P(None, "dp", None, "tp"),
        P(None, "dp", "tp"),
        P(None, None, "tp"),
        P(None, None, None, "tp"),
        P(None, "tp"),
        P(None, "tp"),
        P(None, "tp"),
        P(None, "tp"),
        P(None, "tp", "dp"),
        P(None, "dp", None, "tp"),
        P(None, "dp", None, None, "tp"),
        P(None, "dp", "tp", None, None),
        P(None, "dp", None, "tp"),
    )
    return jax.shard_map(
        functools.partial(body, mesh.shape["tp"], mesh.shape["dp"]),
        mesh=mesh,
        in_specs=placed,
        out_specs=(
            P(None, "dp"),
            P(None, "dp", None, "tp"),
            P(None, "dp", None, None, "tp"),
            P(None, "dp", "tp", None, None),
        ),
        check_vma=False,
    )
```

```python
import functools

import jax
import jax.numpy as jnp
from jax import lax
from jax.experimental import pallas as pl
from jax.experimental.pallas import tpu as pltpu
from jax.sharding import PartitionSpec as P

EPS = 1e-06
LANES = 128
FRONT = 8
F32, BF16 = jnp.float32, jnp.bfloat16


def up(n):
    return -(-n // LANES) * LANES


def dot(a, b, ca=1, cb=0):
    return lax.dot_general(a, b, (((ca,), (cb,)), ((), ())), preferred_element_type=F32)


def thirds(a):
    high = a.astype(BF16)
    rest = a - high.astype(F32)
    middle = rest.astype(BF16)
    return high, middle, (rest - middle.astype(F32)).astype(BF16)


def grid(n_rows, n_cols):
    return (
        lax.broadcasted_iota(jnp.int32, (n_rows, n_cols), 0),
        lax.broadcasted_iota(jnp.int32, (n_rows, n_cols), 1),
    )


def over(a, n):
    return lax.shift_right_logical(a, jnp.full_like(a, n.bit_length() - 1))


def ones_where(cond):
    return jnp.where(cond, 1.0, 0.0).astype(BF16)


def far_first(k, me, n):
    upper = me // (n // 2)
    mirrored = n - 1 - me
    return upper * (k + (k - me + n) // n) + (1 - upper) * (n - 1 - k - (k - mirrored + n) // n)


def kernel(
    n_tp, n_dp, d_model, heads, groups, slots, seqs, hp_cols, map_cols,
    lens, x, scale, w_pair, w_maps, w_step, tap_u, tap_m, bias, rate, skip, gain, cache_u, cache_m, extra_t,
    state_hbm, wout_hbm,
    stream, kept, ssm,
    a_send, a_recv, m_send, m_recv, h_send, h_recv, o_send, o_recv, n_send, n_recv, padded, step_w, state, wout, taps, par, extra,
    a_ss, a_rs, m_ss, m_rs, h_ss, h_rs, o_ss, o_rs, n_ss, n_rs, s_sem, w_sem,
):
    tp, dp = lax.axis_index("tp"), lax.axis_index("dp")
    layers = w_pair.shape[0]
    rows = seqs * slots
    taps_n = tap_u.shape[1]
    keep = taps_n - 1
    zc = up(hp_cols)
    ng = map_cols // groups
    n_state = state.shape[-1]
    cut = stream.shape[0] // n_tp
    per = rows // cut
    head_size = hp_cols // heads

    state_copy = pltpu.make_async_copy(state_hbm, state, s_sem)
    wout_copy = pltpu.make_async_copy(wout_hbm, wout, w_sem)
    state_copy.start()
    wout_copy.start()
    barrier = pltpu.get_barrier_semaphore()
    for k in range(1, n_dp):
        pl.semaphore_signal(barrier, inc=1, device_id={"dp": lax.rem(dp + k, n_dp)})
    for k in range(1, n_tp):
        pl.semaphore_signal(barrier, inc=1, device_id={"tp": lax.rem(tp + k, n_tp)})

    stream[...] = x[...].astype(F32)
    slot = lax.broadcasted_iota(jnp.int32, (slots, 1), 0)
    mask = jnp.concatenate([(slot < lens[s]).astype(F32) for s in range(seqs)], axis=0)
    lane = lax.broadcasted_iota(jnp.int32, (1, LANES), 1)
    r, c = grid(rows, rows)
    causal = (over(r, slots) == over(c, slots)) & (c <= r)
    tri = ones_where(causal)
    r, c = grid(2 * map_cols, up(2 * map_cols))
    which = over(r, ng) & 1
    sel = ones_where(c == which * map_cols + groups * (r & (ng - 1)) + over(r, 2 * ng))
    r, c = grid(n_tp * 2 * ng, 2 * n_state)
    sel2 = ones_where(c == (over(r, ng) & 1) * n_state + over(r, 2 * ng) * ng + (r & (ng - 1)))
    r, c = grid(LANES, hp_cols)
    ex = ones_where(r == over(c, head_size))
    r, c = grid(hp_cols, LANES)
    ext = ones_where(c == over(r, head_size))
    r, c = grid(hp_cols, hp_cols)
    ones = ones_where(over(r, head_size) == over(c, head_size))
    r, c = grid(LANES, 2 * LANES)
    spread = ones_where(c == 2 * r)
    padded[...] = jnp.zeros_like(padded)
    step_w[...] = jnp.zeros_like(step_w)
    taps[...] = jnp.zeros_like(taps)
    par[...] = jnp.zeros_like(par)
    extra[...] = jnp.zeros_like(extra)
    for l in range(layers):
        step_w[l, :heads, :] = w_step[l]
        taps[l, :taps_n, :hp_cols] = tap_u[l].astype(F32)
        for t in range(taps_n):
            pair = tap_m[l, t].astype(F32)
            for which in range(2):
                at = zc + which * map_cols
                taps[l, t : t + 1, at : at + map_cols] = pair[which : which + 1]
        par[l, 0:1, :heads] = bias[l : l + 1, :]
        par[l, 1:2, :heads] = rate[l : l + 1, :]
        par[l, 2:3, :heads] = skip[l : l + 1, :]
        for s in range(seqs):
            extra[l, :heads, s * slots : (s + 1) * slots] = extra_t[l, s]
    extra_rows = [extra[l].T[:rows] for l in range(layers)]
    skip_x = [sum(dot(piece, ex) for piece in thirds(par[l]))[2:3] for l in range(layers)]
    sends = []

    def copy(src, dst, ss, rs, where):
        return pltpu.make_async_remote_copy(
            src_ref=src, dst_ref=dst, send_sem=ss, recv_sem=rs, device_id=where
        )

    for l in range(layers):
        st = stream[...]
        squares = jnp.sum(st * st, axis=1, keepdims=True)
        normed = (st * scale[l : l + 1, :]).astype(BF16)
        even = jnp.concatenate(
            [dot(normed[:, i : i + LANES], spread) for i in range(0, normed.shape[1], LANES)], axis=1
        )
        odd = pltpu.roll(even, 1, 1)
        pair = dot(jnp.concatenate([even.astype(BF16), odd.astype(BF16)], axis=0), w_pair[l])
        tokens = st.shape[0]
        tail = dot(normed, step_w[l], 1, 1)
        high = squares.astype(BF16).astype(F32)
        tail = jnp.where(lane == LANES - 2, high, jnp.where(lane == LANES - 1, squares - high, tail))
        part = jnp.concatenate(
            [pair[:tokens], pair[tokens:], dot(normed, w_maps[l], 1, 1), tail], axis=1
        ).astype(BF16)
        for b in range(n_dp):
            a_send[l, b] = part[b * rows : (b + 1) * rows]
        if l == 0:
            pl.semaphore_wait(barrier, n_dp - 1 + n_tp - 1)
        flights = []
        for k in range(1, n_dp):
            to = lax.rem(dp + k, n_dp)
            c = copy(a_send.at[l, to], a_recv.at[l, k - 1], a_ss.at[l, k - 1], a_rs.at[l, k - 1], {"dp": to})
            c.start()
            flights.append(c)
        sends += flights
        acc = a_send[l, dp].astype(F32)
        for k, c in enumerate(flights):
            c.wait_recv()
            acc = acc + a_recv[l, k].astype(F32)
        tail = acc[:, acc.shape[1] - LANES :]
        squares = tail[:, LANES - 2 : LANES - 1] + tail[:, LANES - 1 : LANES]
        factor = lax.rsqrt(squares / d_model + EPS)
        proj = (acc * factor).astype(BF16).astype(F32)

        conv_w = taps.shape[2]
        pieces = []
        for s in range(seqs):
            for t in range(keep):
                at = FRONT - keep + t
                padded[s, at : at + 1, :hp_cols] = cache_u[l, t].astype(F32)[s : s + 1]
                pair = cache_m[l, s, t].astype(F32)
                for which in range(2):
                    col = zc + which * map_cols
                    padded[s, at : at + 1, col : col + map_cols] = pair[which : which + 1]
            padded[s, FRONT : FRONT + slots, :] = proj[s * slots : (s + 1) * slots, zc : zc + conv_w]
            total = padded[s, FRONT - keep : FRONT - keep + slots, :] * taps[l, 0:1, :]
            for t in range(1, taps_n):
                at = FRONT - keep + t
                total = total + padded[s, at : at + slots, :] * taps[l, t : t + 1, :]
            pieces.append(total)
        filtered = jnp.concatenate(pieces, axis=0)
        filtered = filtered * jax.nn.sigmoid(filtered)
        maps = filtered[:, conv_w - up(2 * map_cols) :].astype(BF16)
        sorted_maps = dot(sel, maps, 1, 1)
        for g in range(groups):
            m_send[l, g] = sorted_maps[g * 2 * ng : (g + 1) * 2 * ng, :].astype(BF16)

        def group_of(rank):
            return rank * heads // (heads * n_tp // groups)

        flights = []
        for k in range(n_tp - 1):
            to = far_first(k, tp, n_tp)
            c = copy(m_send.at[l, group_of(to)], m_recv.at[l, tp], m_ss.at[l, k], m_rs.at[l, tp], {"tp": to})
            c.start()
            sends.append(c)
        m_recv[l, tp] = m_send[l, group_of(tp)]

        for s in range(seqs):
            pick = lax.broadcasted_iota(jnp.int32, (8, FRONT + slots), 0)
            place = lax.broadcasted_iota(jnp.int32, (8, FRONT + slots), 1)
            chooser = ((place == pick + lens[s] + (FRONT - keep)) & (pick < keep)).astype(BF16)
            kept[l, s] = dot(chooser, padded[s].astype(BF16)).astype(BF16)
        raw = proj[:, proj.shape[1] - LANES :] + par[l, 0:1, :]
        step = (jnp.maximum(raw, 0.0) + jnp.log1p(jnp.exp(-jnp.abs(raw)))) * mask
        step = jnp.where(lane < heads, step, 0.0)
        logdec = extra_rows[l] * mask - step * jnp.exp(par[l, 1:2, :])
        logdec = jnp.where(lane < heads, logdec, 0.0)
        parts = dot(tri, jnp.concatenate(thirds(logdec), axis=1))
        sums = parts[:, :LANES] + parts[:, LANES : 2 * LANES] + parts[:, 2 * LANES :]
        sums_t = sums.T
        step_t = step.T
        sums_parts, step_parts = thirds(sums), thirds(step)
        both = dot(jnp.concatenate(sums_parts + step_parts, axis=0), ex)
        sums_x = both[:rows] + both[rows : 2 * rows] + both[2 * rows : 3 * rows]
        step_x = both[3 * rows : 4 * rows] + both[4 * rows : 5 * rows] + both[5 * rows :]
        inp = filtered[:, :hp_cols]
        gate = proj[:, :hp_cols]
        last_x = jnp.concatenate(
            [
                jnp.broadcast_to(sums_x[(s + 1) * slots - 1 : (s + 1) * slots, :], (slots, hp_cols))
                for s in range(seqs)
            ],
            axis=0,
        )
        weighted = (jnp.exp(last_x - sums_x) * step_x * inp).astype(BF16)
        inp_b = inp.astype(BF16)
        grow = jnp.exp(sums_x)
        direct = skip_x[l] * inp
        gate = gate * jax.nn.sigmoid(gate)
        rows_sum = sum(dot(ext, piece, 1, 1) for piece in sums_parts)
        segs = []
        for h in range(heads):
            gap = sums[:, h : h + 1] - sums_t[h : h + 1, :]
            segs.append(jnp.exp(jnp.where(causal, gap, -jnp.inf)) * step_t[h : h + 1, :])

        if l == 0:
            state_copy.wait()
            wout_copy.wait()
        for k in range(1, n_tp):
            src = lax.rem(tp + n_tp - k, n_tp)
            copy(m_send.at[l, 0], m_recv.at[l, src], m_ss.at[l, 0], m_rs.at[l, src], {"tp": src}).wait_recv()
        got = m_recv[l].astype(F32).reshape(n_tp * 2 * ng, rows)
        both_maps = dot(got.T.astype(BF16), sel2).astype(BF16)
        b_map, c_map = both_maps[:, :n_state], both_maps[:, n_state:]
        cross = dot(c_map, b_map, 1, 1)
        within = jnp.concatenate(
            [
                dot((cross * segs[h]).astype(BF16), inp_b[:, h * head_size : (h + 1) * head_size])
                for h in range(heads)
            ],
            axis=1,
        )
        carried = jnp.concatenate(
            [
                dot(c_map[s * slots : (s + 1) * slots], state[l, s].astype(BF16), 1, 1)
                for s in range(seqs)
            ],
            axis=0,
        )
        read = (within + carried * grow + direct) * gate
        power = read * read
        p_hi = power.astype(BF16)
        p_lo = (power - p_hi.astype(F32)).astype(BF16)
        mean = (dot(p_hi, ones) + dot(p_lo, ones)) / head_size
        headout = (read * lax.rsqrt(mean + EPS) * gain[l : l + 1, :] * mask).astype(BF16)
        h_send[l] = headout
        flights = []
        for k in range(1, n_dp):
            to = lax.rem(dp + k, n_dp)
            c = copy(h_send.at[l], h_recv.at[l, k - 1], h_ss.at[l, k - 1], h_rs.at[l, k - 1], {"dp": to})
            c.start()
            flights.append(c)
        sends += flights

        def push(value, block):
            out = dot(value, wout[l]).astype(BF16)
            for i in range(per):
                to = block * per + i
                o_send[l, to] = out[i * cut : (i + 1) * cut]

                @pl.when(to != tp)
                def _():
                    copy(o_send.at[l, to], o_recv.at[l, tp], o_ss.at[l, to], o_rs.at[l, tp], {"tp": to}).start()

        push(headout, dp)
        for s in range(seqs):
            at = slice(s * slots, (s + 1) * slots)
            fresh = dot(weighted[at], b_map[at], 0, 0)
            end = (s + 1) * slots - 1
            ssm[l, s] = jnp.exp(rows_sum[:, end : end + 1]) * state[l, s] + fresh
        for k, c in enumerate(flights):
            c.wait_recv()
            push(h_recv[l, k], lax.rem(dp + n_dp - k - 1, n_dp))
        total = o_send[l, tp].astype(F32)
        for k in range(1, n_tp):
            src = lax.rem(tp + n_tp - k, n_tp)
            copy(o_send.at[l, src], o_recv.at[l, src], o_ss.at[l, src], o_rs.at[l, src], {"tp": src}).wait_recv()
            total = total + o_recv[l, src].astype(F32)
        fresh = total.astype(BF16)
        n_send[l] = fresh
        n_recv[l, tp] = fresh
        for k in range(n_tp - 1):
            to = far_first(k, tp, n_tp)
            c = copy(n_send.at[l], n_recv.at[l, tp], n_ss.at[l, k], n_rs.at[l, tp], {"tp": to})
            c.start()
            sends.append(c)
        for k in range(1, n_tp):
            src = lax.rem(tp + n_tp - k, n_tp)
            copy(n_send.at[l], n_recv.at[l, src], n_ss.at[l, 0], n_rs.at[l, src], {"tp": src}).wait_recv()
        stream[...] += n_recv[l].astype(F32).reshape(stream.shape)

    for c in sends:
        c.wait_send()
    for l in range(layers):
        for k in range(1, n_tp):
            to = lax.rem(tp + k, n_tp)
            copy(o_send.at[l, to], o_recv.at[l, tp], o_ss.at[l, to], o_rs.at[l, tp], {"tp": to}).wait_send()


def body(
    n_tp, n_dp,
    tokens, lengths, input_norm_scale, gate_input_weight, maps_weight, step_weight,
    input_tap_weight, map_tap_weight, step_size_bias, decay_rate_logarithm, direct_path_weight,
    head_norm_scale, output_weight, convolution_input_cache, convolution_map_cache,
    recurrent_state, extra_log_decay,
):
    layers, seqs, slots, heads = extra_log_decay.shape
    head_size, n_state = recurrent_state.shape[3:]
    hp_cols = heads * head_size
    map_cols = maps_weight.shape[3]
    groups = map_cols * n_tp // n_state
    ng = map_cols // groups
    rows = seqs * slots
    d_here = tokens.shape[1]
    keep = convolution_input_cache.shape[2]

    def wide(a):
        pad = up(a.shape[-1]) - a.shape[-1]
        return a if pad == 0 else jnp.pad(a, [(0, 0)] * (a.ndim - 1) + [(0, pad)])

    w_pair = wide(gate_input_weight.reshape(layers, 2 * d_here, hp_cols))
    w_maps = jnp.transpose(maps_weight, (0, 2, 3, 1)).reshape(layers, 2 * map_cols, d_here)
    if up(2 * map_cols) > 2 * map_cols:
        w_maps = jnp.pad(w_maps, ((0, 0), (0, up(2 * map_cols) - 2 * map_cols), (0, 0)))
    w_step = jnp.transpose(step_weight, (0, 2, 1))
    cache_u = jnp.transpose(convolution_input_cache, (0, 2, 1, 3))
    extra_t = jnp.transpose(extra_log_decay, (0, 1, 3, 2))
    state = recurrent_state.reshape(layers, seqs, hp_cols, n_state)

    vmem = pl.BlockSpec(memory_space=pltpu.VMEM)
    wide_cols = 2 * up(hp_cols) + up(2 * map_cols) + LANES
    anywhere = pl.BlockSpec(memory_space=pl.ANY)
    conv_w = up(hp_cols) + up(2 * map_cols)
    cut = tokens.shape[0] // n_tp
    sems = lambda n: pltpu.SemaphoreType.DMA((layers, n))
    args = [tokens, input_norm_scale, w_pair, w_maps, w_step, input_tap_weight,
        map_tap_weight, step_size_bias, decay_rate_logarithm, direct_path_weight, head_norm_scale,
        cache_u, convolution_map_cache, extra_t]
    stream, kept, ssm = pl.pallas_call(
        functools.partial(
            kernel, n_tp, n_dp, d_here * n_dp, heads, groups, slots, seqs, hp_cols, map_cols
        ),
        out_shape=(
            jax.ShapeDtypeStruct(tokens.shape, F32),
            jax.ShapeDtypeStruct((layers, seqs, 8, conv_w), BF16),
            jax.ShapeDtypeStruct(state.shape, F32),
        ),
        in_specs=[pl.BlockSpec(memory_space=pltpu.SMEM)] + [vmem] * len(args) + [anywhere] * 2,
        out_specs=(vmem, vmem, vmem),
        scratch_shapes=[
            pltpu.VMEM((layers, n_dp, rows, wide_cols), BF16),
            pltpu.VMEM((layers, n_dp - 1, rows, wide_cols), BF16),
            pltpu.VMEM((layers, groups, 2 * ng, rows), BF16),
            pltpu.VMEM((layers, n_tp, 2 * ng, rows), BF16),
            pltpu.VMEM((layers, rows, hp_cols), BF16),
            pltpu.VMEM((layers, n_dp - 1, rows, hp_cols), BF16),
            pltpu.VMEM((layers, n_tp, cut, d_here), BF16),
            pltpu.VMEM((layers, n_tp, cut, d_here), BF16),
            pltpu.VMEM((layers, cut, d_here), BF16),
            pltpu.VMEM((layers, n_tp, cut, d_here), BF16),
            pltpu.VMEM((seqs, FRONT + slots, conv_w), F32),
            pltpu.VMEM((layers, LANES, d_here), BF16),
            pltpu.VMEM(state.shape, F32),
            pltpu.VMEM(output_weight.shape, BF16),
            pltpu.VMEM((layers, 8, conv_w), F32),
            pltpu.VMEM((layers, 8, LANES), F32),
            pltpu.VMEM((layers, LANES, LANES), F32),
            sems(n_dp - 1), sems(n_dp - 1), sems(n_tp - 1), sems(n_tp), sems(n_dp - 1),
            sems(n_dp - 1), sems(n_tp), sems(n_tp), sems(n_tp - 1), sems(n_tp),
            pltpu.SemaphoreType.DMA, pltpu.SemaphoreType.DMA,
        ],
        compiler_params=pltpu.CompilerParams(
            collective_id=0, has_side_effects=True, vmem_limit_bytes=48 * 2**20
        ),
        name="mixer",
    )(lengths, *args, state, output_weight)
    conv_in = kept[:, :, :keep, :hp_cols]
    start = conv_w - up(2 * map_cols)
    conv_maps = kept[:, :, :keep, start : start + 2 * map_cols].reshape(
        layers, seqs, keep, 2, map_cols
    )
    return stream, conv_in, conv_maps, ssm.reshape(recurrent_state.shape)


def solution(mesh):
    placed = (
        P(None, "dp"),
        P("dp"),
        P(None, "dp"),
        P(None, "dp", None, "tp"),
        P(None, "dp", None, "tp"),
        P(None, "dp", "tp"),
        P(None, None, "tp"),
        P(None, None, None, "tp"),
        P(None, "tp"),
        P(None, "tp"),
        P(None, "tp"),
        P(None, "tp"),
        P(None, "tp", "dp"),
        P(None, "dp", None, "tp"),
        P(None, "dp", None, None, "tp"),
        P(None, "dp", "tp", None, None),
        P(None, "dp", None, "tp"),
    )
    return jax.shard_map(
        functools.partial(body, mesh.shape["tp"], mesh.shape["dp"]),
        mesh=mesh,
        in_specs=placed,
        out_specs=(
            P(None, "dp"),
            P(None, "dp", None, "tp"),
            P(None, "dp", None, None, "tp"),
            P(None, "dp", "tp", None, None),
        ),
        check_vma=False,
    )
```
